32 devices in a mesh: ep: 8 (over z, x), tp: 4 (over y, core).
Axes of the slice: x: 2, y: 2, z: 4, core: 2. Of those that a mesh axis runs over, the one named last changes fastest.
Arguments:
- mixer_in: bfloat16 [1024, 2048], P('ep'), may hold values from -6 to 6
- mixer_gain: float32 [2048], replicated, may hold values from 0.1 to 1.9
- w_value: bfloat16 [2048, 1536], P(None, 'tp'), may hold values from -0.125 to 0.125
- w_gate: bfloat16 [2048, 1536], P(None, 'tp'), may hold values from -0.125 to 0.125
- w_taps: float32 [31, 1536], P(None, 'tp'), may hold values from -3 to 3
- channel_gain: float32 [1536], P('tp'), may hold values from 0.1 to 1.9
- w_output: bfloat16 [1536, 2048], P('tp'), may hold values from -0.15625 to 0.15625
- expert_in: bfloat16 [1024, 2048], P('ep'), may hold values from -6 to 6
- expert_gain: float32 [2048], replicated, may hold values from 0 to 8
- route_experts: int32 [1024, 4], P('ep'), may hold values from 0 to 7, all different within a row; in each aligned block of 128 rows (0 to 127, 128 to 255, ...) at most 128 rows name the same one
- route_scores: float32 [1024, 4], P('ep'), may hold values from -6 to 6
- expert_gate: bfloat16 [8, 2048, 2048], P('ep', None, 'tp'), may hold values from -0.125 to 0.125
- expert_up: bfloat16 [8, 2048, 2048], P('ep', None, 'tp'), may hold values from -0.125 to 0.125
- expert_down: bfloat16 [8, 2048, 2048], P('ep', 'tp'), may hold values from -0.125 to 0.125
Outputs:
- mixer_out: bfloat16 [1024, 2048], P('ep')
- expert_out: bfloat16 [1024, 2048], P('ep')
The draws below stay inside these ranges and needn't reach their ends.
Inputs may be any that keep to these rules, and one draw needn't show every extreme that they name: `route_experts`: each row names 4 different experts. In each aligned block of 128 rows (the rows of one index of ep) no expert is named more than 128 times, a bound that some block reaches.
All inputs are finite; a program needn't handle non-finite values.
Results may differ from the reference program's by a relative error of at most 0.02.
Values may be sent and summed in bfloat16 or wider, within the bound.
A program may use at most 64 MiB of HBM per device.

```python
import math
import jax
import jax.numpy as jnp
import numpy as np
from jax import lax

D = 2048
CONV_CH = 1536
CONV_W = 31
FF = 2048
TOP_K = 4
TOK = 128
EXPERTS = 8
SEQ = 1024
CAP = 128
CH_DEV = 384
FF_DEV = 512
N_EP = 8


def draw_w_taps(key, part):
    base_key, factor_key = jax.random.split(jax.random.fold_in(key, 17))
    base_taps = jnp.clip(jax.random.normal(base_key, (CONV_W, CONV_CH), jnp.float32), -4.0, 4.0) * CONV_W ** (-0.5)
    factors = jnp.exp(jax.random.uniform(factor_key, (CONV_CH // CH_DEV,), jnp.float32, -math.log(3.0), math.log(3.0)))
    return base_taps * jnp.repeat(factors, CH_DEV)[None, :]


def draw_expert_gain(key, part):
    noise = jnp.clip(jax.random.normal(jax.random.fold_in(key, 29), (D,), jnp.float32), -3.0, 3.0)
    gain_values = 1.0 + 0.18 * noise
    return gain_values


def steps_of(rng, dims, cuts, low, largest):
    def one(dim, parts):
        steps = jax.random.uniform(jax.random.fold_in(jax.random.fold_in(rng, 6), dim), (parts,), jnp.float32, low / len(cuts), largest / len(cuts))
        return jnp.repeat(jnp.exp(steps), dims[dim] // parts).reshape((-1,) + (1,) * (len(dims) - dim - 1))

    level = one(*cuts[0])
    for cut in cuts[1:]:
        level = level * one(*cut)
    return level


def assign_block(key, own, number, rows, count, top, reach, skew):
    sequence = jax.random.permutation(key, count)
    heavy_load, ordinary = portions_of(count, rows * top, reach, skew, True), portions_of(count, rows * top, reach, skew, False)
    places = jnp.arange(count)

    def named(sizes, rotation):
        used = int((sizes > 0).sum())
        fixed = max(1, used // 4)
        moved = fixed + (places - fixed + rotation * (used - fixed)) % max(1, count - fixed)
        return jnp.zeros((count,), jnp.int32).at[sequence[jnp.where(places < fixed, places, moved)]].set(jnp.asarray(sizes, jnp.int32))

    sizes = jnp.where(number % 4 == 0, named(heavy_load, number // 4), named(ordinary, number - number // 4 - 1))
    mixed = jax.random.permutation(jax.random.fold_in(own, 3), count)
    giver, receiver = mixed[0:count // 2 * 2:2], mixed[1:count // 2 * 2:2]
    room = jnp.minimum(sizes[giver] - 1, reach - sizes[receiver]) // 2
    room = jnp.where((giver == sequence[0]) | (receiver == sequence[0]) | (sizes[receiver] == 0), 0, jnp.maximum(room, 0))
    moved = jax.random.randint(jax.random.fold_in(own, 4), (count // 2,), 0, 1 << 20) % (room + 1)
    sizes = sizes.at[giver].add(-moved).at[receiver].add(moved)
    members = jnp.searchsorted(jnp.cumsum(sizes), jnp.arange(rows * top), side="right").astype(jnp.int32)
    grid = members.reshape(top, rows).T
    grid = grid[jax.random.permutation(jax.random.fold_in(own, 1), rows)]
    rotation = jax.random.randint(jax.random.fold_in(own, 2), (rows, 1), 0, top)
    return jnp.take_along_axis(grid, (jnp.arange(top)[None, :] + rotation) % top, axis=1)


def portions_of(count, total, most, slope, full):
    weights = [(1 << 20) // math.isqrt(rank ** slope) + 1 for rank in range(1, count + 1)]
    largest = most if full else min(most, max(-(-total // count), total * weights[0] // sum(weights)))
    least = 1 if total - largest >= count - 1 else 0
    given, spare = [largest] + [least] * (count - 1), total - largest - least * (count - 1)
    while spare > 0:
        candidates = [i for i in range(1, count) if given[i] < largest] or [i for i in range(1, count) if given[i] < most]
        pool, budget = sum([weights[i] for i in candidates]), spare
        for i in candidates:
            addition = min(most - given[i], max(1, budget * weights[i] // pool), spare)
            given[i] = given[i] + addition
            spare = spare - addition
    return np.array(given)


def centred(key, shape, scale, reach, cuts=(), kind=jnp.bfloat16):
    factor_of = steps_of(key, shape, cuts, -0.22, 0.18) if cuts else 1.0
    drawn = jax.random.normal(key, shape, jnp.float32) * scale * factor_of
    return jnp.minimum(jnp.maximum(drawn, -reach), reach).astype(kind)


def setup_inputs(seed: int = 0) -> dict:
    streams_of = jax.random.split(jax.random.key(seed), 15)
    mixer_in = centred(streams_of[0], (SEQ, D), 1.0, 6.0, ((0, 8),))
    mixer_gain = jnp.clip(1.0 + 0.18 * jax.random.normal(streams_of[1], (D,), jnp.float32), 0.1, 1.9)
    w_value = centred(streams_of[2], (D, CONV_CH), D ** -0.5, 0.125, ((1, 4),))
    w_gate = centred(streams_of[3], (D, CONV_CH), D ** -0.5, 0.125, ((1, 4),))
    w_taps = draw_w_taps(jax.random.fold_in(streams_of[14], 71), 0)
    channel_gain = jnp.clip(1.0 + 0.18 * jax.random.normal(streams_of[5], (CONV_CH,), jnp.float32), 0.1, 1.9)
    w_output = centred(streams_of[6], (CONV_CH, D), CONV_CH ** -0.5, 0.15625, ((0, 4),))
    expert_in = centred(streams_of[7], (SEQ, D), 1.0, 6.0, ((0, 8),))
    expert_gain = draw_expert_gain(jax.random.fold_in(streams_of[14], 71), 0)
    route_experts_keys = jax.random.split(jax.random.fold_in(streams_of[9], 1), SEQ // TOK)
    route_experts_turns = jax.random.permutation(jax.random.fold_in(streams_of[9], 3), SEQ // TOK)
    route_experts = jax.vmap(lambda own, number: assign_block(jax.random.fold_in(streams_of[9], 2), own, number, TOK, EXPERTS, TOP_K, CAP, 1))(route_experts_keys, route_experts_turns).reshape((SEQ, TOP_K))
    route_scores = centred(streams_of[10], (SEQ, TOP_K), 1.0, 6.0, ((0, 8),), jnp.float32)
    expert_gate = centred(streams_of[11], (EXPERTS, D, FF), D ** -0.5, 0.125, ((0, 8), (2, 4)))
    expert_up = centred(streams_of[12], (EXPERTS, D, FF), D ** -0.5, 0.125, ((0, 8), (2, 4)))
    expert_down = centred(streams_of[13], (EXPERTS, FF, D), FF ** -0.5, 0.125, ((0, 8), (1, 4)))
    return {"mixer_in": mixer_in, "mixer_gain": mixer_gain, "w_value": w_value, "w_gate": w_gate, "w_taps": w_taps, "channel_gain": channel_gain, "w_output": w_output, "expert_in": expert_in, "expert_gain": expert_gain, "route_experts": route_experts, "route_scores": route_scores, "expert_gate": expert_gate, "expert_up": expert_up, "expert_down": expert_down}


epsilon = 1e-05
clamp_limit = 7.0
swish_slope = 1.702

def row_norm(inputs, gains):
    widened = inputs.astype(jnp.float32)
    row_mean = lax.optimization_barrier(jnp.mean(widened, axis=-1, keepdims=True))
    row_var = lax.optimization_barrier(jnp.mean(jnp.square(widened - row_mean), axis=-1, keepdims=True))
    return (widened - row_mean) * lax.rsqrt(row_var + epsilon) * gains

def mixer_half(mixer_in, mixer_gain, w_value, w_gate, w_taps, channel_gain, w_output):
    normed = row_norm(mixer_in, mixer_gain).astype(jnp.bfloat16)
    values = jnp.dot(normed, w_value, preferred_element_type=jnp.float32)
    gate_pre = jnp.dot(normed, w_gate, preferred_element_type=jnp.float32)
    gated_values = (values * jax.nn.sigmoid(gate_pre)).astype(jnp.bfloat16)
    extended = jnp.concatenate([jnp.zeros((CONV_W - 1, CONV_CH), jnp.bfloat16), gated_values], axis=0)
    conv_out = jnp.zeros((SEQ, CONV_CH), jnp.float32)
    for offset in range(CONV_W):
        conv_out = conv_out + extended[offset:offset + SEQ].astype(jnp.float32) * w_taps[offset]
    row_mean = lax.optimization_barrier(jnp.sum(conv_out, axis=1, keepdims=True)) / CONV_CH
    row_var = lax.optimization_barrier(jnp.sum(conv_out * conv_out, axis=1, keepdims=True)) / CONV_CH - row_mean * row_mean
    activated = jax.nn.silu((conv_out - row_mean) * lax.rsqrt(row_var + epsilon) * channel_gain).astype(jnp.bfloat16)
    summed = jnp.zeros((SEQ, D), jnp.float32)
    for block_index in range(CONV_CH // CH_DEV):
        first_col = block_index * CH_DEV
        block_term = jnp.dot(activated[:, first_col:first_col + CH_DEV], w_output[first_col:first_col + CH_DEV], preferred_element_type=jnp.float32)
        summed = summed + lax.optimization_barrier(block_term.astype(jnp.bfloat16)).astype(jnp.float32)
    return summed.astype(jnp.bfloat16)

def expert_half(expert_in, expert_gain, route_experts, route_scores, expert_gate, expert_up, expert_down):
    normed = row_norm(expert_in, expert_gain).astype(jnp.bfloat16)
    raised = jnp.exp(route_scores)
    route_weights = raised / lax.optimization_barrier(jnp.sum(raised, axis=1, keepdims=True))
    chosen = route_experts.reshape(N_EP, TOK * TOP_K).astype(jnp.int32)
    onehot = (chosen[:, :, None] == jnp.arange(EXPERTS, dtype=jnp.int32)[None, None, :]).astype(jnp.int32)
    slot_index = lax.optimization_barrier(jnp.sum((jnp.cumsum(onehot, axis=1) - onehot) * onehot, axis=2)).astype(jnp.int32)
    source = jnp.arange(N_EP, dtype=jnp.int32)[:, None]
    owner_row = (source * TOK + jnp.arange(TOK * TOP_K, dtype=jnp.int32)[None, :] // TOP_K).astype(jnp.int32)
    placed = ((chosen * N_EP + source) * CAP + slot_index).reshape(-1).astype(jnp.int32)
    slot_table = jnp.full((EXPERTS * N_EP * CAP,), SEQ, jnp.int32).at[placed].set(owner_row.reshape(-1))
    padded = jnp.concatenate([normed, jnp.zeros((1, D), jnp.bfloat16)], axis=0)

    def one_expert(operands):
        table_rows, gate_w, up_w, down_w = operands
        gathered = padded[table_rows.astype(jnp.int32)]
        gate_pre = jnp.minimum(jnp.dot(gathered, gate_w, preferred_element_type=jnp.float32), clamp_limit)
        up_pre = jnp.clip(jnp.dot(gathered, up_w, preferred_element_type=jnp.float32), -clamp_limit, clamp_limit)
        hidden = ((up_pre + 1.0) * gate_pre * jax.nn.sigmoid(swish_slope * gate_pre)).astype(jnp.bfloat16)
        summed = jnp.zeros((N_EP * CAP, D), jnp.float32)
        for block_index in range(FF // FF_DEV):
            first_col = block_index * FF_DEV
            block_term = jnp.dot(hidden[:, first_col:first_col + FF_DEV], down_w[first_col:first_col + FF_DEV], preferred_element_type=jnp.float32)
            summed = summed + lax.optimization_barrier(block_term.astype(jnp.bfloat16)).astype(jnp.float32)
        return summed.astype(jnp.bfloat16)
    expert_rows = lax.map(one_expert, (slot_table.reshape(EXPERTS, N_EP * CAP), expert_gate, expert_up, expert_down))
    picked = expert_rows.reshape(EXPERTS * N_EP * CAP, D)[placed].astype(jnp.float32).reshape(SEQ, TOP_K, D)
    return lax.optimization_barrier(jnp.sum(picked * route_weights[:, :, None], axis=1)).astype(jnp.bfloat16)

def reference(mixer_in, mixer_gain, w_value, w_gate, w_taps, channel_gain, w_output, expert_in, expert_gain, route_experts, route_scores, expert_gate, expert_up, expert_down):
    mixer_out = mixer_half(mixer_in, mixer_gain, w_value, w_gate, w_taps, channel_gain, w_output)
    expert_out = expert_half(expert_in, expert_gain, route_experts, route_scores, expert_gate, expert_up, expert_down)
    return (mixer_out, expert_out)
```

```python
import functools

import jax
import jax.numpy as jnp
from jax import lax
from jax.experimental import pallas as pl
from jax.experimental.pallas import tpu as pltpu
from jax.sharding import PartitionSpec as P

CONV_CH = 1536
CONV_W = 31
TOP_K = 4


epsilon = 1e-05
clamp_limit = 7.0
swish_slope = 1.702


def shifted(block, axis, distance):
    devices = range(lax.axis_size(axis))
    route = [(i - distance, i) for i in devices if i - distance in devices]
    return lax.ppermute(block, axis, route)


def row_norm(inputs, gains):
    widened = inputs.astype(jnp.float32)
    row_mean = jnp.mean(widened, axis=-1, keepdims=True)
    row_var = jnp.mean(jnp.square(widened - row_mean), axis=-1, keepdims=True)
    return (widened - row_mean) * lax.rsqrt(row_var + epsilon) * gains


def local(
    mixer_in,
    mixer_gain,
    w_value,
    w_gate,
    w_taps,
    channel_gain,
    w_output,
    expert_in,
    expert_gain,
    route_experts,
    route_scores,
    expert_gate,
    expert_up,
    expert_down,
):
    normed = row_norm(mixer_in, mixer_gain).astype(jnp.bfloat16)
    values = jnp.dot(normed, w_value, preferred_element_type=jnp.float32)
    gate_pre = jnp.dot(normed, w_gate, preferred_element_type=jnp.float32)
    gated_values = (values * jax.nn.sigmoid(gate_pre)).astype(jnp.bfloat16)
    mixer_rows = gated_values.shape[0]
    reach_rows = CONV_W - 1
    earlier = shifted(gated_values[mixer_rows - reach_rows :], "ep", 1)
    extended = jnp.concatenate([earlier, gated_values], axis=0)
    conv_out = jnp.zeros(gated_values.shape, jnp.float32)
    for offset in range(CONV_W):
        conv_out = (
            conv_out + extended[offset : offset + mixer_rows].astype(jnp.float32) * w_taps[offset]
        )
    channel_sums = lax.psum(
        (
            jnp.sum(conv_out, axis=1, keepdims=True),
            jnp.sum(conv_out * conv_out, axis=1, keepdims=True),
        ),
        "tp",
    )
    row_mean = channel_sums[0] / CONV_CH
    row_var = channel_sums[1] / CONV_CH - row_mean * row_mean
    activated = jax.nn.silu(
        (conv_out - row_mean) * lax.rsqrt(row_var + epsilon) * channel_gain
    ).astype(jnp.bfloat16)
    mixer_out = lax.psum(
        jnp.dot(activated, w_output, preferred_element_type=jnp.float32).astype(jnp.bfloat16), "tp"
    )
    rows_b = expert_in.shape[0]
    width = expert_in.shape[1]
    experts = lax.axis_size("ep")
    capacity = 2 * rows_b * TOP_K // experts
    slot_share = capacity // lax.axis_size("tp")
    column = lax.axis_index("tp")
    normed_b = row_norm(expert_in, expert_gain).astype(jnp.bfloat16)
    raised = jnp.exp(route_scores)
    route_weights = raised / jnp.sum(raised, axis=1, keepdims=True)
    flat_ids = route_experts.reshape(-1)
    onehot = (flat_ids[:, None] == jnp.arange(experts, dtype=jnp.int32)[None, :]).astype(jnp.int32)
    slot_index = jnp.sum((jnp.cumsum(onehot, axis=0) - onehot) * onehot, axis=1)
    owner_row = jnp.arange(rows_b * TOP_K, dtype=jnp.int32) // TOP_K
    slot_table = (
        jnp.full((capacity * experts,), rows_b, jnp.int32)
        .at[slot_index * experts + flat_ids]
        .set(owner_row)
    )
    padded = jnp.concatenate([normed_b, jnp.zeros((1, width), jnp.bfloat16)], axis=0)
    gate_w = expert_gate[0]
    up_w = expert_up[0]
    down_w = expert_down[0]
    own_table = lax.dynamic_slice_in_dim(
        slot_table, column * slot_share * experts, slot_share * experts
    )
    sending = jnp.take(padded, own_table, axis=0).reshape(slot_share, experts, width)
    arrived = lax.all_to_all(sending, "ep", split_axis=1, concat_axis=1, tiled=True)
    block_rows = lax.all_gather(arrived, "tp", axis=0, tiled=True)
    flat_rows = block_rows.reshape(block_rows.shape[0] * block_rows.shape[1], block_rows.shape[2])
    gate_e = jnp.minimum(
        jnp.dot(flat_rows, gate_w, preferred_element_type=jnp.float32), clamp_limit
    )
    up_e = jnp.clip(
        jnp.dot(flat_rows, up_w, preferred_element_type=jnp.float32), -clamp_limit, clamp_limit
    )
    hidden = (
        ((up_e + 1.0) * gate_e * jax.nn.sigmoid(swish_slope * gate_e))
        .astype(jnp.bfloat16)
        .reshape(block_rows.shape[0], block_rows.shape[1], gate_w.shape[1])
        .reshape(capacity * experts, gate_w.shape[1])
    )
    summed = lax.psum_scatter(
        jnp.dot(hidden, down_w, preferred_element_type=jnp.float32).astype(jnp.bfloat16),
        "tp",
        scatter_dimension=0,
        tiled=True,
    )
    returned = lax.all_to_all(
        summed.reshape(slot_share, experts, width), "ep", split_axis=1, concat_axis=1, tiled=True
    )
    every_slot = lax.all_gather(returned, "tp", axis=0, tiled=True).reshape(
        capacity * experts, width
    )
    picked = jnp.take(every_slot, slot_index * experts + flat_ids, axis=0)
    picked = picked.reshape(rows_b, TOP_K, width).astype(jnp.float32)
    expert_out = jnp.sum(picked * route_weights[:, :, None], axis=1).astype(jnp.bfloat16)
    return (mixer_out, expert_out)


MESH = pl.DeviceIdType.MESH
QUARTERS = 4
HALO = 32


def kernel(
    ep,
    tp,
    mixer_in,
    mixer_gain,
    w_value,
    w_gate,
    w_taps,
    channel_gain,
    w_output,
    expert_in,
    expert_gain,
    route_experts,
    route_scores,
    expert_gate,
    expert_up,
    expert_down,
    mixer_out,
    expert_out,
    wv,
    wg,
    wo,
    eg,
    eu,
    ed,
    load_sem,
    send_sem,
    recv_sem,
    tokens,
    shares,
    gated_tail,
    halo,
    extended,
    conv,
    stats,
    mixer_part,
    mixer_core,
    mixer_y,
    mixer_all,
    hidden,
    parts,
    part_core,
    part_y,
    part_x,
    part_ring,
    expert_y,
    expert_all,
):
    rows = mixer_in.shape[0]
    width = mixer_in.shape[1] // QUARTERS
    depth = ep // 2
    me = lax.axis_index("ep")
    col = lax.axis_index("tp")
    z, x = lax.div(me, 2), lax.rem(me, 2)
    y, core = lax.div(col, 2), lax.rem(col, 2)
    z_next = (lax.rem(z + 1, depth) * 2 + x, col)
    x_peer = (z * 2 + 1 - x, col)
    y_peer = (me, (1 - y) * 2 + core)
    core_peer = (me, y * 2 + 1 - core)
    own_q, other_q = 2 * core + y, 2 * core + 1 - y
    own_half, other_half = pl.ds(2 * core, 2), pl.ds(2 * (1 - core), 2)
    f32, bf16 = jnp.float32, jnp.bfloat16

    def behind(steps):
        return lax.rem(z + depth - steps, depth)

    sent = []

    def send(src, dst, device):
        i = len(sent)
        copy = pltpu.make_async_remote_copy(
            src_ref=src,
            dst_ref=dst,
            send_sem=send_sem.at[i],
            recv_sem=recv_sem.at[i],
            device_id=device,
            device_id_type=MESH,
        )
        copy.start()
        sent.append(copy)
        return copy

    barrier = pltpu.get_barrier_semaphore()
    for d in range(1, ep):
        pl.semaphore_signal(
            barrier, inc=1, device_id=(lax.rem(me + d, ep), col), device_id_type=MESH
        )
    for d in range(1, tp):
        pl.semaphore_signal(
            barrier, inc=1, device_id=(me, lax.rem(col + d, tp)), device_id_type=MESH
        )

    loads = [
        pltpu.make_async_copy(src, dst, load_sem.at[i])
        for i, (src, dst) in enumerate(
            (
                (w_value, wv),
                (w_gate, wg),
                (w_output, wo),
                (expert_gate.at[0], eg),
                (expert_up.at[0], eu),
                (expert_down.at[0], ed),
            )
        )
    ]
    for load in loads:
        load.start()

    def norm(ref, gain):
        widened = ref[...].astype(f32)
        mean = jnp.mean(widened, axis=-1, keepdims=True)
        centred = widened - mean
        var = jnp.mean(centred * centred, axis=-1, keepdims=True)
        return (centred * lax.rsqrt(var + epsilon) * gain[...]).astype(bf16)

    normed = norm(expert_in, expert_gain)
    for q in range(QUARTERS):
        tokens[me, q] = normed[:, q * width : (q + 1) * width]
    raised = jnp.exp(route_scores[...])
    weights = raised / jnp.sum(raised, axis=1, keepdims=True)
    ids = route_experts[...]
    lane = lax.broadcasted_iota(jnp.int32, (rows, rows), 1)
    dense = jnp.zeros((rows, rows), f32)
    for k in range(TOP_K):
        dense = dense + jnp.where(ids[:, k : k + 1] == lane, weights[:, k : k + 1], 0.0)
    shares[me] = jnp.transpose(dense)[:ep]
    pl.semaphore_wait(barrier, ep - 1 + tp - 1)

    z_copies, x_copies, y_copies, cz_copies, cx_copies = [], [], [], [None], []

    def send_z(block):
        part = tokens.at[block, own_half]
        z_copies.append(send(part, part, z_next))

    def send_x(block):
        part = tokens.at[block, own_q]
        x_copies.append(send(part, part, x_peer))

    def send_core(block, copies):
        part = tokens.at[block, own_half]
        copies.append(send(part, part, core_peer))

    send_x(me)
    send_z(me)
    share_copies = [
        send(shares.at[me], shares.at[me], (lax.rem(me + d, ep), col)) for d in range(1, ep)
    ]

    def arrived_z(step):
        block = behind(step) * 2 + x
        z_copies[step - 1].wait_recv()
        if step < depth - 1:
            send_z(block)
        send_x(block)
        send_core(block, cz_copies)

    def arrived_x(step):
        x_copies[step].wait_recv()
        part = tokens.at[behind(step) * 2 + 1 - x, own_q]
        y_copies.append(send(part, part, y_peer))

    def arrived_y(step):
        y_copies[step].wait_recv()
        send_core(behind(step) * 2 + 1 - x, cx_copies)

    def share_column(block):
        row = shares[block, pl.ds(me, 1), :]
        return jnp.transpose(jnp.broadcast_to(row, (rows, rows)))[:, :1]

    ret_core = []

    def expert_step(step):
        if step:
            cz_copies[step].wait_recv()
        cx_copies[step].wait_recv()
        first = behind(step) * 2
        blocks = pl.ds(first, 2)
        inputs = jnp.concatenate(
            [tokens[blocks, q].reshape(2 * rows, width) for q in range(QUARTERS)], axis=1
        )
        share = jnp.concatenate([share_column(first), share_column(first + 1)], axis=0)
        chunk = min(256, eg.shape[1])
        for n in range(0, eg.shape[1], chunk):
            gate_e = jnp.minimum(
                jnp.dot(inputs, eg[:, n : n + chunk], preferred_element_type=f32), clamp_limit
            )
            up_e = jnp.clip(
                jnp.dot(inputs, eu[:, n : n + chunk], preferred_element_type=f32),
                -clamp_limit,
                clamp_limit,
            )
            act = (up_e + 1.0) * gate_e * jax.nn.sigmoid(swish_slope * gate_e)
            hidden[:, n : n + chunk] = (act * share).astype(bf16)
        for q in range(QUARTERS):
            down = jnp.dot(
                hidden[...], ed[:, q * width : (q + 1) * width], preferred_element_type=f32
            )
            parts[blocks, q] = down.astype(bf16).reshape(2, rows, width)
        ret_core.append(send(parts.at[blocks, other_half], part_core.at[behind(step)], core_peer))

    ret_y, ret_x, ring = {}, {}, []

    def add_to(block, q, term):
        parts[block, q] = (parts[block, q].astype(f32) + term.astype(f32)).astype(bf16)

    def return_core(step):
        zi = behind(step)
        ret_core[step].wait_recv()
        for b in range(2):
            for h in range(2):
                add_to(2 * zi + b, 2 * core + h, part_core[zi, b, h])
        ret_y[step] = send(parts.at[2 * zi + 1 - x, other_q], part_y.at[zi], y_peer)

    def return_y(step):
        zi = behind(step)
        ret_y[step].wait_recv()
        add_to(2 * zi + 1 - x, own_q, part_y[zi])
        ret_x[step] = send(parts.at[2 * zi + 1 - x, own_q], part_x.at[zi], x_peer)

    def return_x(step):
        zi = behind(step)
        ret_x[step].wait_recv()
        add_to(2 * zi + x, own_q, part_x[zi])

    def ring_step(step):
        block = 2 * behind(step) + x
        if step > 1:
            ring[step - 2].wait_recv()
            for h in range(2):
                add_to(block, 2 * core + h, part_ring[step - 2, h])
        ring.append(send(parts.at[block, own_half], part_ring.at[step - 1], z_next))

    loads[0].wait()
    loads[1].wait()
    normed_a = norm(mixer_in, mixer_gain)
    values = jnp.dot(normed_a, wv[...], preferred_element_type=f32)
    gate_pre = jnp.dot(normed_a, wg[...], preferred_element_type=f32)
    gated = (values * jax.nn.sigmoid(gate_pre)).astype(bf16)
    gated_tail[...] = gated[rows - HALO :]
    extended[pl.ds(HALO, rows), :] = gated.astype(f32)
    halo_copy = send(gated_tail, halo, (lax.rem(me + 1, ep), col))

    arrived_x(0)

    halo_copy.wait_recv()
    keep = jnp.where(me > 0, 1.0, 0.0).astype(f32)
    extended[pl.ds(0, HALO), :] = halo[...].astype(f32) * keep
    channels = w_taps.shape[1]
    sums = jnp.zeros((rows, 1), f32)
    squares = jnp.zeros((rows, 1), f32)
    first = HALO - (CONV_W - 1)
    for c in range(0, channels, 128):
        total = jnp.zeros((rows, 128), f32)
        for offset in range(CONV_W):
            total = (
                total
                + extended[pl.ds(first + offset, rows), c : c + 128]
                * w_taps[offset : offset + 1, c : c + 128]
            )
        conv[:, c : c + 128] = total
        sums = sums + jnp.sum(total, axis=1, keepdims=True)
        squares = squares + jnp.sum(total * total, axis=1, keepdims=True)
    stats[0] = jnp.transpose(jnp.where(lane == 0, sums, jnp.where(lane == 1, squares, 0.0)))[:8]
    stat_copies = [
        send(stats.at[0], stats.at[d], (me, lax.rem(col + d, tp))) for d in range(1, tp)
    ]

    arrived_z(1)
    arrived_y(0)

    for copy in stat_copies:
        copy.wait_recv()
    stat = stats[0]
    for d in range(1, tp):
        stat = stat + stats[d]
    stat = jnp.transpose(jnp.concatenate([stat] * (rows // 8), axis=0))
    row_mean = stat[:, 0:1] / CONV_CH
    row_var = stat[:, 1:2] / CONV_CH - row_mean * row_mean
    activated = jax.nn.silu(
        (conv[...] - row_mean) * lax.rsqrt(row_var + epsilon) * channel_gain[...]
    ).astype(bf16)
    loads[2].wait()
    for q in range(QUARTERS):
        mixer_part[q] = jnp.dot(
            activated, wo[:, q * width : (q + 1) * width], preferred_element_type=f32
        ).astype(bf16)
    m_core = send(mixer_part.at[other_half], mixer_core, core_peer)

    for copy in share_copies:
        copy.wait_recv()
    for load in loads[3:]:
        load.wait()
    expert_step(0)

    def mixer_sum():
        m_core.wait_recv()
        for h in range(2):
            q = 2 * core + h
            mixer_part[q] = (mixer_part[q].astype(f32) + mixer_core[h].astype(f32)).astype(bf16)
        return send(mixer_part.at[other_q], mixer_y, y_peer)

    def spread_y(whole):
        return send(whole.at[own_q], whole.at[own_q], y_peer)

    def spread_core(whole):
        return send(whole.at[own_half], whole.at[own_half], core_peer)

    arrived_x(1)
    m_y = mixer_sum()
    for step in range(1, depth):
        if step < depth - 1:
            arrived_z(step + 1)
        arrived_y(step)
        return_core(step - 1)
        if step >= 2:
            return_y(step - 2)
        expert_step(step)
        if step < depth - 1:
            arrived_x(step + 1)
        if step == 1:
            m_y.wait_recv()
            mixer_all[own_q] = (mixer_part[own_q].astype(f32) + mixer_y[...].astype(f32)).astype(
                bf16
            )
            m_spread = spread_y(mixer_all)
        if step == 2:
            m_spread.wait_recv()
            m_last = spread_core(mixer_all)
        if step >= 3:
            return_x(step - 2)
            ring_step(step - 2)

    last = depth - 1
    return_y(last - 1)
    return_core(last)
    return_x(last - 1)
    ring_step(last - 1)
    return_y(last)
    return_x(0)
    m_last.wait_recv()
    for q in range(QUARTERS):
        mixer_out[:, q * width : (q + 1) * width] = mixer_all[q]
    return_x(last)
    ring_step(last)
    ring[last - 1].wait_recv()
    for h in range(2):
        add_to(me, 2 * core + h, part_ring[last - 1, h])
    e_y = send(parts.at[me, other_q], expert_y, y_peer)
    e_y.wait_recv()
    expert_all[own_q] = (parts[me, own_q].astype(f32) + expert_y[...].astype(f32)).astype(bf16)
    spread_y(expert_all).wait_recv()
    spread_core(expert_all).wait_recv()
    for q in range(QUARTERS):
        expert_out[:, q * width : (q + 1) * width] = expert_all[q]
    for copy in sent:
        copy.wait_send()


def fused_local(sizes, *args):
    ep, tp = sizes["ep"], sizes["tp"]
    mixer_in, w_value, w_taps, w_output = args[0], args[2], args[4], args[6]
    expert_in, gate_w = args[7], args[11]
    rows, features = expert_in.shape
    capacity = 2 * rows * TOP_K // ep
    if capacity < rows or tp != 4 or ep != 8 or rows != 128:
        return local(*args)
    width = features // QUARTERS
    depth = ep // 2
    hidden_units = gate_w.shape[2]
    channels = w_taps.shape[1]
    f32, bf16 = jnp.float32, jnp.bfloat16
    vmem = pl.BlockSpec(memory_space=pltpu.VMEM)
    hbm = pl.BlockSpec(memory_space=pl.ANY)
    copies = 96
    tile = (rows, width)
    args = list(args)
    for i in (1, 5, 8):
        args[i] = args[i].reshape(1, -1)
    flops = 2 * rows * ep * features * hidden_units * 3
    return pl.pallas_call(
        functools.partial(kernel, ep, tp),
        out_shape=(
            jax.ShapeDtypeStruct(mixer_in.shape, bf16),
            jax.ShapeDtypeStruct(expert_in.shape, bf16),
        ),
        in_specs=[hbm if i in (2, 3, 6, 11, 12, 13) else vmem for i in range(14)],
        out_specs=(vmem, vmem),
        scratch_shapes=[
            pltpu.VMEM(w_value.shape, bf16),
            pltpu.VMEM(w_value.shape, bf16),
            pltpu.VMEM(w_output.shape, bf16),
            pltpu.VMEM((features, hidden_units), bf16),
            pltpu.VMEM((features, hidden_units), bf16),
            pltpu.VMEM((hidden_units, features), bf16),
            pltpu.SemaphoreType.DMA((6,)),
            pltpu.SemaphoreType.DMA((copies,)),
            pltpu.SemaphoreType.DMA((copies,)),
            pltpu.VMEM((ep, QUARTERS) + tile, bf16),
            pltpu.VMEM((ep, ep, rows), f32),
            pltpu.VMEM((HALO, channels), bf16),
            pltpu.VMEM((HALO, channels), bf16),
            pltpu.VMEM((HALO + rows, channels), f32),
            pltpu.VMEM((rows, channels), f32),
            pltpu.VMEM((tp, 8, rows), f32),
            pltpu.VMEM((QUARTERS,) + tile, bf16),
            pltpu.VMEM((2,) + tile, bf16),
            pltpu.VMEM(tile, bf16),
            pltpu.VMEM((QUARTERS,) + tile, bf16),
            pltpu.VMEM((2 * rows, hidden_units), bf16),
            pltpu.VMEM((ep, QUARTERS) + tile, bf16),
            pltpu.VMEM((depth, 2, 2) + tile, bf16),
            pltpu.VMEM((depth,) + tile, bf16),
            pltpu.VMEM((depth,) + tile, bf16),
            pltpu.VMEM((depth - 1, 2) + tile, bf16),
            pltpu.VMEM(tile, bf16),
            pltpu.VMEM((QUARTERS,) + tile, bf16),
        ],
        compiler_params=pltpu.CompilerParams(
            collective_id=0, has_side_effects=True, vmem_limit_bytes=56 * 1024 * 1024
        ),
        cost_estimate=pl.CostEstimate(flops=flops, bytes_accessed=1 << 24, transcendentals=0),
        name="mixer_and_experts",
    )(*args)


def solution(mesh):
    body = functools.partial(fused_local, dict(mesh.shape))
    in_specs = (
        P("ep", None),
        P(),
        P(None, "tp"),
        P(None, "tp"),
        P(None, "tp"),
        P("tp"),
        P("tp", None),
        P("ep", None),
        P(),
        P("ep", None),
        P("ep", None),
        P("ep", None, "tp"),
        P("ep", None, "tp"),
        P("ep", "tp", None),
    )
    out_specs = (P("ep", None), P("ep", None))
    return jax.shard_map(body, mesh=mesh, in_specs=in_specs, out_specs=out_specs, check_vma=False)
```
